32 devices in a mesh: ep: 8 (over z, y), tp: 4 (over x, core).
Axes of the slice: x: 2, y: 2, z: 4, core: 2. Of those that a mesh axis runs over, the one named last changes fastest.
Arguments:
- tokens: bfloat16 [1024, 2048], P('ep'), may hold values from -36 to 36, as said below
- norm_gain: float32 [2048], replicated, may hold values from 0.1 to 1.9
- chosen: int32 [8, 256], replicated, may hold values from 0 to 1023, as said below
- slot_weight: float32 [8, 256], replicated, may hold values from 0.1 to 1
- gate_weight: bfloat16 [8, 2048, 4096], P(None, 'ep', 'tp'), may hold values from -0.125 to 0.125
- up_weight: bfloat16 [8, 2048, 4096], P(None, 'ep', 'tp'), may hold values from -0.125 to 0.125
- down_weight: bfloat16 [8, 2048, 4096], P(None, 'ep', 'tp'), may hold values from -0.09375 to 0.09375
Outputs:
- mixed: bfloat16 [1024, 2048], P('ep', 'tp')
The draws below stay inside these ranges and needn't reach their ends.
Inputs may be any that keep to these rules, and one draw needn't show every extreme that they name: `tokens`: each entry is the scaled entry of a bounded draw; rows and features differ in scale. `chosen`: the 256 slots of an expert name distinct tokens. Slots of an expert fall into aligned blocks of 256; within a block the token numbers ascend, and at most 64 of them lie among the 128 tokens of one index of ep (tokens i * 128 onward belong to index i); in every block some index supplies exactly 64.
All inputs are finite; a program needn't handle non-finite values.
Results may differ from the reference program's by a relative error of at most 0.019.
Values may be sent and summed in bfloat16 or wider, within the bound.
A program may use at most 64 MiB of HBM per device.

```python
import math
import jax
import jax.numpy as jnp
from jax import lax

D = 2048
FF = 4096
EXPERTS = 8
TOK_DEV = 128
TOKENS = 1024
CAP = 256
SLOTS_DEV = 256
SLOT_CAP = 64
N_TP = 4


def draw_tokens(key, part):
    row_key, column_key, base_key = jax.random.split(jax.random.fold_in(key, 3), 3)
    row_scale = jnp.exp(jax.random.uniform(row_key, (TOKENS, 1), jnp.float32, math.log(0.3), math.log(3.0)))
    column_scale = jnp.exp(jax.random.uniform(column_key, (1, D), jnp.float32, math.log(0.3), math.log(3.0)))
    base = jax.random.normal(base_key, (TOKENS, D), jnp.float32)
    base = jnp.clip(base, -4.0, 4.0)
    return (base * row_scale * column_scale).astype(jnp.bfloat16)


def draw_chosen(key, part):
    owners_total = TOKENS // TOK_DEV
    group_size = owners_total // EXPERTS
    seats_total = owners_total * SLOT_CAP
    order_key, seat_key, forced_key = jax.random.split(jax.random.fold_in(key, 17), 3)
    order_scores = jax.random.randint(order_key, (EXPERTS, owners_total, TOK_DEV), 0, 1 << 20) * TOK_DEV
    order_scores = order_scores + jnp.arange(TOK_DEV, dtype=jnp.int32)
    token_order = jnp.argsort(order_scores, axis=-1).astype(jnp.int32)
    seat_scores = jax.random.randint(seat_key, (owners_total, seats_total), 0, 1 << 20) * seats_total
    seat_scores = seat_scores + jnp.arange(seats_total, dtype=jnp.int32)
    forced_owner = jax.random.randint(forced_key, (owners_total, 1), 0, owners_total)
    seat_owner_all = jnp.arange(seats_total, dtype=jnp.int32) // SLOT_CAP
    seat_scores = jnp.where(seat_owner_all[None, :] == forced_owner, seat_scores - (1 << 30), seat_scores)
    picked_seats = jnp.argsort(seat_scores, axis=-1)[:, :SLOTS_DEV].astype(jnp.int32)
    seat_owner = picked_seats // SLOT_CAP
    seat_rank = picked_seats % SLOT_CAP
    piece_index = jnp.arange(owners_total, dtype=jnp.int32)[:, None]
    expert_index = piece_index // group_size
    within = piece_index % group_size * SLOT_CAP + seat_rank
    local_token = token_order[expert_index, seat_owner, within]
    global_token = seat_owner * TOK_DEV + local_token
    return jnp.sort(global_token, axis=-1).reshape(EXPERTS, CAP).astype(jnp.int32)


def steps_of(rng, dims, cuts, least, largest):
    def one(position, shards_of):
        heights = jax.random.uniform(jax.random.fold_in(jax.random.fold_in(rng, 6), position), (shards_of,), jnp.float32, least / len(cuts), largest / len(cuts))
        return jnp.repeat(jnp.exp(heights), dims[position] // shards_of).reshape((-1,) + (1,) * (len(dims) - position - 1))

    factor_of = one(*cuts[0])
    for cut in cuts[1:]:
        factor_of = factor_of * one(*cut)
    return factor_of


def noise(key, dims, deviation, reach, shards=(), kind=jnp.bfloat16):
    values = jax.random.normal(key, dims, jnp.float32) * deviation
    if len(shards) > 0:
        values = steps_of(key, dims, shards, -0.22, 0.18) * values
    return jnp.clip(values, min=-reach, max=reach).astype(kind)


def setup_inputs(seed: int = 0) -> dict:
    key_of = jax.random.split(jax.random.key(seed), 8)
    return {
        "tokens": draw_tokens(jax.random.fold_in(key_of[7], 71), 0),
        "norm_gain": jnp.clip(1.0 + 0.18 * jax.random.normal(key_of[1], (D,), jnp.float32), 0.1, 1.9),
        "chosen": draw_chosen(jax.random.fold_in(key_of[7], 71), 0),
        "slot_weight": jnp.clip(jnp.exp(jax.random.uniform(key_of[3], (EXPERTS, CAP), jnp.float32, math.log(0.1), math.log(1.0))), 0.1, 1.0),
        "gate_weight": noise(key_of[4], (EXPERTS, D, FF), D ** -0.5, 0.125, ((1, 8), (2, 4))),
        "up_weight": noise(key_of[5], (EXPERTS, D, FF), D ** -0.5, 0.125, ((1, 8), (2, 4))),
        "down_weight": noise(key_of[6], (EXPERTS, D, FF), FF ** -0.5, 0.09375, ((1, 8), (2, 4))),
    }


EPSILON = 1e-06

def reference(tokens, norm_gain, chosen, slot_weight, gate_weight, up_weight, down_weight):
    values = tokens.astype(jnp.float32)
    scaled = values * lax.rsqrt(lax.optimization_barrier(jnp.mean(values * values, axis=1, keepdims=True)) + EPSILON)
    normed = (scaled * norm_gain).astype(jnp.bfloat16)
    block_units = FF // N_TP

    def per_expert(accumulated, operands):
        picked, weights, gate_w, up_w, down_w = operands
        gathered = jnp.take(normed, picked, axis=0)
        gate_part = jnp.dot(gathered, gate_w, preferred_element_type=jnp.float32)
        up_part = jnp.dot(gathered, up_w, preferred_element_type=jnp.float32)
        hidden = (jax.nn.silu(gate_part) * up_part).astype(jnp.bfloat16)

        def add_block(running, block_index):
            hidden_block = lax.dynamic_slice_in_dim(hidden, block_index * block_units, block_units, 1)
            down_block = lax.dynamic_slice_in_dim(down_w, block_index * block_units, block_units, 1)
            partial_value = jnp.dot(hidden_block, down_block.T, preferred_element_type=jnp.float32).astype(jnp.bfloat16)
            partial_value = lax.optimization_barrier(partial_value)
            return (running + partial_value.astype(jnp.float32), None)
        summed, _ = lax.scan(add_block, jnp.zeros((CAP, D), jnp.float32), jnp.arange(N_TP, dtype=jnp.int32))
        expert_out = summed.astype(jnp.bfloat16)
        contribution = weights[:, None] * expert_out.astype(jnp.float32)
        return (accumulated.at[picked].add(contribution), None)
    mixed_out, _ = lax.scan(per_expert, jnp.zeros((TOKENS, D), jnp.float32), (chosen, slot_weight, gate_weight, up_weight, down_weight))
    return mixed_out.astype(jnp.bfloat16)
```

```python
import functools

import jax
import jax.numpy as jnp
from jax import lax
from jax.experimental import pallas as pl
from jax.experimental.pallas import tpu as pltpu
from jax.sharding import PartitionSpec as P

EPSILON = 1e-06
MESH = pl.DeviceIdType.MESH
F32 = jnp.float32
BF16 = jnp.bfloat16


def kernel(
    n, n_tp, slots, tokens_ref, gain_ref, chosen_ref, weight_ref, gate_hbm, up_hbm, down_hbm, out_ref,
    gate_v, up_v, down_v, nbuf, xall, xs, sbuf, rbuf, hbuf, mix, obuf, fbuf,
    w_sem, d_send, d_recv, r_send, r_recv, g_send, g_recv, f_send, f_recv,
):
    experts, depth, ff = gate_v.shape
    rows = tokens_ref.shape[0]
    subs, width = sbuf.shape[1], sbuf.shape[3]
    half = subs // 2
    group = n // experts
    ratio = n // n_tp
    me = lax.axis_index("ep")
    col = lax.axis_index("tp")

    odd = me % 2
    pos = (1 - odd) * (me // 2) + odd * (n - 1 - me // 2)

    def index_at(position):
        p = (position + 2 * n) % n
        late = p // (n // 2)
        return (1 - late) * 2 * p + late * (2 * (n - 1 - p) + 1)

    neighbour = (index_at(pos + 1), index_at(pos - 1))
    owner_col = me // ratio
    own_slot = (me % ratio) * n_tp + col
    selfish = (owner_col == col).astype(jnp.int32)

    barrier = pltpu.get_barrier_semaphore()

    def greet(j, _):
        pl.semaphore_signal(barrier, inc=1, device_id=((me + j) % n, col), device_id_type=MESH)
        return 0

    lax.fori_loop(1, n, greet, 0)

    def greet_out(j, _):
        target = (me + j) % n
        source_row = col * ratio + j // n_tp
        source_col = j % n_tp

        @pl.when((target != me) | (owner_col != col))
        def _():
            pl.semaphore_signal(barrier, inc=1, device_id=(target, owner_col), device_id_type=MESH)

        @pl.when((source_row != me) | (source_col != col))
        def _():
            pl.semaphore_signal(barrier, inc=1, device_id=(source_row, source_col), device_id_type=MESH)

        return 0

    lax.fori_loop(0, n, greet_out, 0)

    loads = [
        pltpu.make_async_copy(gate_hbm, gate_v, w_sem.at[0]),
        pltpu.make_async_copy(up_hbm, up_v, w_sem.at[1]),
        pltpu.make_async_copy(down_hbm, down_v, w_sem.at[2]),
    ]
    for load in loads:
        load.start()

    values = tokens_ref[...].astype(F32)
    scale = lax.rsqrt(jnp.mean(values * values, axis=1, keepdims=True) + EPSILON)
    normed = (values * scale * gain_ref[...]).astype(BF16)
    for j in range(n):
        nbuf[j] = normed[:, j * depth : (j + 1) * depth]

    pl.semaphore_wait(barrier, (n - 1) + 2 * (n - selfish))

    def dispatch(target, source):
        return pltpu.make_async_remote_copy(
            src_ref=nbuf.at[target], dst_ref=xall.at[source], send_sem=d_send.at[target],
            recv_sem=d_recv.at[source], device_id=(target, col), device_id_type=MESH,
        )

    def send_tokens(j, _):
        dispatch((me + j) % n, me).start()
        return 0

    lax.fori_loop(1, n, send_tokens, 0)
    xall[me] = nbuf[me]
    mix[...] = jnp.zeros_like(mix)

    def wait_tokens(j, _):
        source = (me + n - j) % n
        pltpu.make_async_copy(nbuf.at[source], xall.at[source], d_recv.at[source]).wait()
        return 0

    lax.fori_loop(1, n, wait_tokens, 0)

    def piece_row(ref, q):
        start = pl.multiple_of((q % group) * slots, slots)
        return ref[pl.ds(q // group, 1), pl.ds(start, slots)]

    blocks = n * rows // 128
    step_blocks = min(blocks, 8)

    def gather(q):
        picked = jnp.transpose(jnp.broadcast_to(piece_row(chosen_ref, q), (128, slots)))
        lanes = lax.broadcasted_iota(jnp.int32, (slots, 128), 1)
        total = jnp.zeros((slots, depth), F32)
        per = step_blocks * 128 // rows
        for b in range(0, blocks, step_blocks):
            onehot = jnp.concatenate(
                [jnp.where(picked == lanes + (b + c) * 128, 1.0, 0.0).astype(BF16) for c in range(step_blocks)], axis=1
            )
            first = b * 128 // rows
            part = xall[first : first + per].reshape(step_blocks * 128, depth)
            total = total + jnp.dot(onehot, part, preferred_element_type=F32)
        xs[q] = total.astype(BF16)

    weights = (gate_v, up_v)

    def partial(direction, q, sub):
        w = weights[direction][q // group, :, sub * width : (sub + 1) * width]
        return jnp.dot(xs[q], w, preferred_element_type=F32)

    def reduce_copy(direction, src, step, sub):
        return pltpu.make_async_remote_copy(
            src_ref=src, dst_ref=rbuf.at[direction, step, sub], send_sem=r_send.at[direction, step, sub],
            recv_sem=r_recv.at[direction, step, sub], device_id=(neighbour[direction], col), device_id_type=MESH,
        )

    def chunk(direction, step):
        return index_at(pos - 1 - step) if direction == 0 else index_at(pos + 1 + step)

    gather(chunk(0, 0))
    gather(chunk(1, 0))
    loads[0].wait()
    loads[1].wait()
    for sub in range(subs):
        for direction in range(2):
            sbuf[direction, sub] = partial(direction, chunk(direction, 0), sub).astype(BF16)
            reduce_copy(direction, sbuf.at[direction, sub], 0, sub).start()

    def gather_rest(j, _):
        gather(index_at(pos - 1 - j))
        return 0

    lax.fori_loop(1, n - 2, gather_rest, 0)
    gather(me)

    def reduce_step(step, _):
        for sub in range(subs):
            for direction in range(2):
                mine = partial(direction, chunk(direction, step), sub)
                here = rbuf.at[direction, step - 1, sub]
                reduce_copy(direction, here, step - 1, sub).wait_recv()
                here[...] = (here[...].astype(F32) + mine).astype(BF16)
                reduce_copy(direction, here, step, sub).start()
        return 0

    lax.fori_loop(1, n - 1, reduce_step, 0)

    def spread_copy(direction, source, step, sub):
        block = hbuf.at[source, sub]
        return pltpu.make_async_remote_copy(
            src_ref=block, dst_ref=block, send_sem=g_send.at[step, sub], recv_sem=g_recv.at[step, sub],
            device_id=(neighbour[direction], col), device_id_type=MESH,
        )

    slot_scale = jnp.transpose(jnp.broadcast_to(piece_row(weight_ref, me), (128, slots)))
    slot_scale = jnp.concatenate([slot_scale] * (width // 128), axis=1)
    order = [s for pair in zip(range(half), range(half, subs)) for s in pair]
    for sub in order:
        parts = []
        for direction in range(2):
            mine = partial(direction, me, sub)
            here = rbuf.at[direction, n - 2, sub]
            reduce_copy(direction, here, n - 2, sub).wait_recv()
            parts.append(here[...].astype(F32) + mine)
        hbuf[me, sub] = (parts[0] / (1.0 + jnp.exp(-parts[0])) * parts[1] * slot_scale).astype(BF16)
        spread_copy(sub // half, me, 0, sub).start()
    loads[2].wait()

    def project(q, direction):
        total = jnp.zeros((slots, depth), F32)
        for sub in range(direction * half, (direction + 1) * half):
            w = down_v[q // group, :, sub * width : (sub + 1) * width]
            total = total + lax.dot_general(
                hbuf[q, sub], w, (((1,), (1,)), ((), ())), preferred_element_type=F32
            )
        picked = piece_row(chosen_ref, q)
        value = total.astype(BF16)
        size = step_blocks * 128
        for b in range(0, n * rows, size):
            numbers = lax.broadcasted_iota(jnp.int32, (size, slots), 0) + b
            onehot = jnp.where(numbers == picked, 1.0, 0.0).astype(BF16)
            mix[b : b + size] += jnp.dot(onehot, value, preferred_element_type=F32)

    project(me, 0)
    project(me, 1)

    def spread_step(step, _):
        for direction in range(2):
            source = chunk(direction, step - 1)
            for sub in range(direction * half, (direction + 1) * half):
                spread_copy(direction, source, step - 1, sub).wait_recv()

                @pl.when(step < n - 1)
                def _():
                    spread_copy(direction, source, step, sub).start()

        for direction in range(2):
            project(chunk(direction, step - 1), direction)
        return 0

    lax.fori_loop(1, n, spread_step, 0)

    def final_copy(target, slot):
        return pltpu.make_async_remote_copy(
            src_ref=obuf.at[target], dst_ref=fbuf.at[slot], send_sem=f_send.at[target],
            recv_sem=f_recv.at[slot], device_id=(target, owner_col), device_id_type=MESH,
        )

    def send_out(j, _):
        target = (me + j) % n
        start = pl.multiple_of(target * rows, rows)
        obuf[target] = mix[pl.ds(start, rows), :].astype(BF16)
        away = (target != me) | (owner_col != col)

        @pl.when(away)
        def _():
            final_copy(target, own_slot).start()

        @pl.when(jnp.logical_not(away))
        def _():
            fbuf[own_slot] = obuf[target]

        return 0

    lax.fori_loop(0, n, send_out, 0)

    def sent_tokens(j, _):
        dispatch((me + j) % n, me).wait_send()
        return 0

    lax.fori_loop(1, n, sent_tokens, 0)

    def sent_ring(step, _):
        for sub in range(subs):
            for direction in range(2):
                reduce_copy(direction, sbuf.at[direction, sub], step, sub).wait_send()
            spread_copy(sub // half, me, step, sub).wait_send()
        return 0

    lax.fori_loop(0, n - 1, sent_ring, 0)

    def arrive(j, _):
        source_row = col * ratio + j // n_tp
        source_col = j % n_tp

        @pl.when((source_row != me) | (source_col != col))
        def _():
            pltpu.make_async_copy(obuf.at[0], fbuf.at[j], f_recv.at[j]).wait()

        return 0

    lax.fori_loop(0, n, arrive, 0)
    for b in range(ratio):
        total = fbuf[b * n_tp].astype(F32)
        for k in range(1, n_tp):
            total = total + fbuf[b * n_tp + k].astype(F32)
        out_ref[:, b * depth : (b + 1) * depth] = total.astype(BF16)

    def sent_out(j, _):
        target = (me + j) % n

        @pl.when((target != me) | (owner_col != col))
        def _():
            final_copy(target, own_slot).wait_send()

        return 0

    lax.fori_loop(0, n, sent_out, 0)


def body(tokens, norm_gain, chosen, slot_weight, gate_weight, up_weight, down_weight):
    n = lax.axis_size("ep")
    n_tp = lax.axis_size("tp")
    rows, model_width = tokens.shape
    experts, depth, ff = gate_weight.shape
    slots = chosen.shape[0] * chosen.shape[1] // n
    width = max(128, ff // 4)
    subs = ff // width
    vmem = pl.BlockSpec(memory_space=pltpu.VMEM)
    anywhere = pl.BlockSpec(memory_space=pl.ANY)
    dma = pltpu.SemaphoreType.DMA
    return pl.pallas_call(
        functools.partial(kernel, n, n_tp, slots),
        out_shape=jax.ShapeDtypeStruct((rows, model_width // n_tp), BF16),
        in_specs=[vmem] * 4 + [anywhere] * 3,
        out_specs=vmem,
        scratch_shapes=[
            pltpu.VMEM((experts, depth, ff), BF16),
            pltpu.VMEM((experts, depth, ff), BF16),
            pltpu.VMEM((experts, depth, ff), BF16),
            pltpu.VMEM((n, rows, depth), BF16),
            pltpu.VMEM((n, rows, depth), BF16),
            pltpu.VMEM((n, slots, depth), BF16),
            pltpu.VMEM((2, subs, slots, width), BF16),
            pltpu.VMEM((2, n - 1, subs, slots, width), BF16),
            pltpu.VMEM((n, subs, slots, width), BF16),
            pltpu.VMEM((n * rows, depth), F32),
            pltpu.VMEM((n, rows, depth), BF16),
            pltpu.VMEM((n, rows, depth), BF16),
            dma((3,)),
            dma((n,)),
            dma((n,)),
            dma((2, n - 1, subs)),
            dma((2, n - 1, subs)),
            dma((n - 1, subs)),
            dma((n - 1, subs)),
            dma((n,)),
            dma((n,)),
        ],
        compiler_params=pltpu.CompilerParams(
            collective_id=0, has_side_effects=True, vmem_limit_bytes=64 * 1024 * 1024 - 96 * 1024
        ),
    )(tokens, norm_gain.reshape(1, model_width), chosen, slot_weight, gate_weight, up_weight, down_weight)


def solution(mesh):
    in_specs = (
        P("ep", None),
        P(),
        P(),
        P(),
        P(None, "ep", "tp"),
        P(None, "ep", "tp"),
        P(None, "ep", "tp"),
    )
    out_specs = P("ep", "tp")
    return jax.shard_map(body, mesh=mesh, in_specs=in_specs, out_specs=out_specs, check_vma=False)
```

```python
import functools

import jax
import jax.numpy as jnp
from jax import lax
from jax.experimental import pallas as pl
from jax.experimental.pallas import tpu as pltpu
from jax.sharding import PartitionSpec as P

EPSILON = 1e-06
MESH = pl.DeviceIdType.MESH
F32 = jnp.float32
BF16 = jnp.bfloat16


def kernel(
    n, n_tp, slots, tokens_ref, gain_ref, chosen_ref, weight_ref, gate_hbm, up_hbm, down_hbm, out_ref,
    gate_v, up_v, down_v, nbuf, xall, xs, sbuf, rbuf, hbuf, mix, obuf, pbuf, sumbuf, fbuf,
    w_sem, d_send, d_recv, c_send, c_recv, r_send, r_recv, g_send, g_recv, p_send, p_recv, f_send, f_recv,
):
    experts, depth, ff = gate_v.shape
    rows = tokens_ref.shape[0]
    subs, width = sbuf.shape[1], sbuf.shape[3]
    half = subs // 2
    group = n // experts
    ratio = n // n_tp
    me = lax.axis_index("ep")
    col = lax.axis_index("tp")

    odd = me % 2
    pos = (1 - odd) * (me // 2) + odd * (n - 1 - me // 2)

    def index_at(position):
        p = (position + 2 * n) % n
        late = p // (n // 2)
        return (1 - late) * 2 * p + late * (2 * (n - 1 - p) + 1)

    neighbour = (index_at(pos + 1), index_at(pos - 1))
    owner_col = me // ratio
    core = col % 2
    partner = col + 1 - 2 * core
    pairs = n_tp // 2
    own_slot = (me % ratio) * pairs + col // 2
    part_rows = rows // 2
    selfish = ((owner_col == col) & (me % 2 == core)).astype(jnp.int32)

    barrier = pltpu.get_barrier_semaphore()

    def greet(j, _):
        pl.semaphore_signal(barrier, inc=1, device_id=((me + j) % n, col), device_id_type=MESH)
        return 0

    lax.fori_loop(1, n, greet, 0)

    pl.semaphore_signal(barrier, inc=1, device_id=(me, partner), device_id_type=MESH)

    def owner_at(j):
        return ((me // 2 + j) % (n // 2)) * 2 + core

    def source_at(j):
        return col * ratio + j // pairs, (j % pairs) * 2 + me % 2

    def greet_out(j, _):
        target = owner_at(j)
        source_row, source_col = source_at(j)

        @pl.when((target != me) | (owner_col != col))
        def _():
            pl.semaphore_signal(barrier, inc=1, device_id=(target, owner_col), device_id_type=MESH)

        @pl.when((source_row != me) | (source_col != col))
        def _():
            pl.semaphore_signal(barrier, inc=1, device_id=(source_row, source_col), device_id_type=MESH)

        return 0

    lax.fori_loop(0, n // 2, greet_out, 0)

    loads = [
        pltpu.make_async_copy(gate_hbm, gate_v, w_sem.at[0]),
        pltpu.make_async_copy(up_hbm, up_v, w_sem.at[1]),
        pltpu.make_async_copy(down_hbm, down_v, w_sem.at[2]),
    ]
    for load in loads:
        load.start()

    my_rows = pl.ds(pl.multiple_of(core * part_rows, part_rows), part_rows)
    values = tokens_ref[my_rows, :].astype(F32)
    scale = lax.rsqrt(jnp.mean(values * values, axis=1, keepdims=True) + EPSILON)
    normed = (values * scale * gain_ref[...]).astype(BF16)
    for j in range(n):
        nbuf[j] = normed[:, j * depth : (j + 1) * depth]

    pl.semaphore_wait(barrier, n + 2 * (n // 2 - selfish))

    def dispatch(target, source):
        return pltpu.make_async_remote_copy(
            src_ref=nbuf.at[target], dst_ref=xall.at[source, core], send_sem=d_send.at[target],
            recv_sem=d_recv.at[source], device_id=(target, col), device_id_type=MESH,
        )

    def share(src, source, half_index):
        return pltpu.make_async_remote_copy(
            src_ref=src, dst_ref=xall.at[source, half_index], send_sem=c_send.at[source],
            recv_sem=c_recv.at[source], device_id=(me, partner), device_id_type=MESH,
        )

    def send_tokens(j, _):
        dispatch((me + j) % n, me).start()
        return 0

    lax.fori_loop(1, n, send_tokens, 0)
    share(nbuf.at[me], me, core).start()
    xall[me, core] = nbuf[me]
    mix[...] = jnp.zeros_like(mix)

    def pass_tokens(j, _):
        source = (me + n - j) % n
        dispatch(me, source).wait_recv()
        share(xall.at[source, core], source, core).start()
        return 0

    lax.fori_loop(1, n, pass_tokens, 0)

    def wait_tokens(j, _):
        source = (me + n - j) % n
        share(xall.at[source, core], source, 1 - core).wait_recv()
        return 0

    lax.fori_loop(0, n, wait_tokens, 0)

    def piece_row(ref, q):
        start = pl.multiple_of((q % group) * slots, slots)
        return ref[pl.ds(q // group, 1), pl.ds(start, slots)]

    blocks = n * rows // 128
    step_blocks = min(blocks, 8)

    def gather(q):
        picked = jnp.transpose(jnp.broadcast_to(piece_row(chosen_ref, q), (128, slots)))
        lanes = lax.broadcasted_iota(jnp.int32, (slots, 128), 1)
        total = jnp.zeros((slots, depth), F32)
        per = step_blocks * 128 // rows
        for b in range(0, blocks, step_blocks):
            onehot = jnp.concatenate(
                [jnp.where(picked == lanes + (b + c) * 128, 1.0, 0.0).astype(BF16) for c in range(step_blocks)], axis=1
            )
            first = b * 128 // rows
            part = xall[first : first + per].reshape(step_blocks * 128, depth)
            total = total + jnp.dot(onehot, part, preferred_element_type=F32)
        xs[q] = total.astype(BF16)

    weights = (gate_v, up_v)

    def partial(direction, q, sub):
        w = weights[direction][q // group, :, sub * width : (sub + 1) * width]
        return jnp.dot(xs[q], w, preferred_element_type=F32)

    def reduce_copy(direction, src, step, sub):
        return pltpu.make_async_remote_copy(
            src_ref=src, dst_ref=rbuf.at[direction, step, sub], send_sem=r_send.at[direction, step, sub],
            recv_sem=r_recv.at[direction, step, sub], device_id=(neighbour[direction], col), device_id_type=MESH,
        )

    def chunk(direction, step):
        return index_at(pos - 1 - step) if direction == 0 else index_at(pos + 1 + step)

    gather(chunk(0, 0))
    gather(chunk(1, 0))
    loads[0].wait()
    loads[1].wait()
    for sub in range(subs):
        for direction in range(2):
            sbuf[direction, sub] = partial(direction, chunk(direction, 0), sub).astype(BF16)
            reduce_copy(direction, sbuf.at[direction, sub], 0, sub).start()

    def gather_rest(j, _):
        gather(index_at(pos - 1 - j))
        return 0

    lax.fori_loop(1, n - 2, gather_rest, 0)
    gather(me)

    def reduce_step(step, _):
        for sub in range(subs):
            for direction in range(2):
                mine = partial(direction, chunk(direction, step), sub)
                here = rbuf.at[direction, step - 1, sub]
                reduce_copy(direction, here, step - 1, sub).wait_recv()
                here[...] = (here[...].astype(F32) + mine).astype(BF16)
                reduce_copy(direction, here, step, sub).start()
        return 0

    lax.fori_loop(1, n - 1, reduce_step, 0)

    def spread_copy(direction, source, step, sub):
        block = hbuf.at[source, sub]
        return pltpu.make_async_remote_copy(
            src_ref=block, dst_ref=block, send_sem=g_send.at[step, sub], recv_sem=g_recv.at[step, sub],
            device_id=(neighbour[direction], col), device_id_type=MESH,
        )

    slot_scale = jnp.transpose(jnp.broadcast_to(piece_row(weight_ref, me), (128, slots)))
    slot_scale = jnp.concatenate([slot_scale] * (width // 128), axis=1)
    order = [s for pair in zip(range(half), range(half, subs)) for s in pair]
    for sub in order:
        parts = []
        for direction in range(2):
            mine = partial(direction, me, sub)
            here = rbuf.at[direction, n - 2, sub]
            reduce_copy(direction, here, n - 2, sub).wait_recv()
            parts.append(here[...].astype(F32) + mine)
        hbuf[me, sub] = (parts[0] / (1.0 + jnp.exp(-parts[0])) * parts[1] * slot_scale).astype(BF16)
        spread_copy(sub // half, me, 0, sub).start()
    loads[2].wait()

    def project(q, direction):
        total = jnp.zeros((slots, depth), F32)
        for sub in range(direction * half, (direction + 1) * half):
            w = down_v[q // group, :, sub * width : (sub + 1) * width]
            total = total + lax.dot_general(
                hbuf[q, sub], w, (((1,), (1,)), ((), ())), preferred_element_type=F32
            )
        picked = piece_row(chosen_ref, q)
        value = total.astype(BF16)
        size = step_blocks * 128
        for b in range(0, n * rows, size):
            numbers = lax.broadcasted_iota(jnp.int32, (size, slots), 0) + b
            onehot = jnp.where(numbers == picked, 1.0, 0.0).astype(BF16)
            mix[b : b + size] += jnp.dot(onehot, value, preferred_element_type=F32)

    project(me, 0)
    project(me, 1)

    def spread_step(step, _):
        for direction in range(2):
            source = chunk(direction, step - 1)
            for sub in range(direction * half, (direction + 1) * half):
                spread_copy(direction, source, step - 1, sub).wait_recv()

                @pl.when(step < n - 1)
                def _():
                    spread_copy(direction, source, step, sub).start()

        for direction in range(2):
            project(chunk(direction, step - 1), direction)
        return 0

    lax.fori_loop(1, n, spread_step, 0)

    def pair_copy(j):
        return pltpu.make_async_remote_copy(
            src_ref=obuf.at[j], dst_ref=pbuf.at[j], send_sem=p_send.at[j],
            recv_sem=p_recv.at[j], device_id=(me, partner), device_id_type=MESH,
        )

    def final_copy(j, slot):
        return pltpu.make_async_remote_copy(
            src_ref=sumbuf.at[j], dst_ref=fbuf.at[slot], send_sem=f_send.at[j],
            recv_sem=f_recv.at[slot], device_id=(owner_at(j), owner_col), device_id_type=MESH,
        )

    def mix_rows(target):
        return mix[pl.ds(pl.multiple_of(target * rows, rows), rows), :]

    def send_pair(j, _):
        obuf[j] = mix_rows(owner_at(j) + 1 - 2 * core).astype(BF16)
        pair_copy(j).start()
        return 0

    lax.fori_loop(0, n // 2, send_pair, 0)

    def send_out(j, _):
        target = owner_at(j)
        pair_copy(j).wait_recv()
        sumbuf[j] = (mix_rows(target) + pbuf[j].astype(F32)).astype(BF16)
        away = (target != me) | (owner_col != col)

        @pl.when(away)
        def _():
            final_copy(j, own_slot).start()

        @pl.when(jnp.logical_not(away))
        def _():
            fbuf[own_slot] = sumbuf[j]

        return 0

    lax.fori_loop(0, n // 2, send_out, 0)

    def sent_tokens(j, _):
        source = (me + j) % n
        share(xall.at[source, core], source, core).wait_send()

        @pl.when(j > 0)
        def _():
            dispatch(source, me).wait_send()

        return 0

    lax.fori_loop(0, n, sent_tokens, 0)

    def sent_ring(step, _):
        for sub in range(subs):
            for direction in range(2):
                reduce_copy(direction, sbuf.at[direction, sub], step, sub).wait_send()
            spread_copy(sub // half, me, step, sub).wait_send()
        return 0

    lax.fori_loop(0, n - 1, sent_ring, 0)

    def arrive(j, _):
        source_row, source_col = source_at(j)

        @pl.when((source_row != me) | (source_col != col))
        def _():
            final_copy(0, j).wait_recv()

        return 0

    lax.fori_loop(0, n // 2, arrive, 0)
    for b in range(ratio):
        total = fbuf[b * pairs].astype(F32)
        for k in range(1, pairs):
            total = total + fbuf[b * pairs + k].astype(F32)
        out_ref[:, b * depth : (b + 1) * depth] = total.astype(BF16)

    def sent_out(j, _):
        pair_copy(j).wait_send()

        @pl.when((owner_at(j) != me) | (owner_col != col))
        def _():
            final_copy(j, own_slot).wait_send()

        return 0

    lax.fori_loop(0, n // 2, sent_out, 0)


def body(tokens, norm_gain, chosen, slot_weight, gate_weight, up_weight, down_weight):
    n = lax.axis_size("ep")
    n_tp = lax.axis_size("tp")
    rows, model_width = tokens.shape
    experts, depth, ff = gate_weight.shape
    slots = chosen.shape[0] * chosen.shape[1] // n
    width = max(128, ff // 4)
    subs = ff // width
    vmem = pl.BlockSpec(memory_space=pltpu.VMEM)
    anywhere = pl.BlockSpec(memory_space=pl.ANY)
    dma = pltpu.SemaphoreType.DMA
    return pl.pallas_call(
        functools.partial(kernel, n, n_tp, slots),
        out_shape=jax.ShapeDtypeStruct((rows, model_width // n_tp), BF16),
        in_specs=[vmem] * 4 + [anywhere] * 3,
        out_specs=vmem,
        scratch_shapes=[
            pltpu.VMEM((experts, depth, ff), BF16),
            pltpu.VMEM((experts, depth, ff), BF16),
            pltpu.VMEM((experts, depth, ff), BF16),
            pltpu.VMEM((n, rows // 2, depth), BF16),
            pltpu.VMEM((n, 2, rows // 2, depth), BF16),
            pltpu.VMEM((n, slots, depth), BF16),
            pltpu.VMEM((2, subs, slots, width), BF16),
            pltpu.VMEM((2, n - 1, subs, slots, width), BF16),
            pltpu.VMEM((n, subs, slots, width), BF16),
            pltpu.VMEM((n * rows, depth), F32),
            pltpu.VMEM((n // 2, rows, depth), BF16),
            pltpu.VMEM((n // 2, rows, depth), BF16),
            pltpu.VMEM((n // 2, rows, depth), BF16),
            pltpu.VMEM((n // 2, rows, depth), BF16),
            dma((3,)),
            dma((n,)),
            dma((n,)),
            dma((n,)),
            dma((n,)),
            dma((2, n - 1, subs)),
            dma((2, n - 1, subs)),
            dma((n - 1, subs)),
            dma((n - 1, subs)),
            dma((n // 2,)),
            dma((n // 2,)),
            dma((n // 2,)),
            dma((n // 2,)),
        ],
        compiler_params=pltpu.CompilerParams(
            collective_id=0, has_side_effects=True, vmem_limit_bytes=64 * 1024 * 1024 - 96 * 1024
        ),
    )(tokens, norm_gain.reshape(1, model_width), chosen, slot_weight, gate_weight, up_weight, down_weight)


def solution(mesh):
    in_specs = (
        P("ep", None),
        P(),
        P(),
        P(),
        P(None, "ep", "tp"),
        P(None, "ep", "tp"),
        P(None, "ep", "tp"),
    )
    out_specs = P("ep", "tp")
    return jax.shard_map(body, mesh=mesh, in_specs=in_specs, out_specs=out_specs, check_vma=False)
```

```python
import functools

import jax
import jax.numpy as jnp
from jax import lax
from jax.experimental import pallas as pl
from jax.experimental.pallas import tpu as pltpu
from jax.sharding import PartitionSpec as P

EPSILON = 1e-06
MESH = pl.DeviceIdType.MESH
F32 = jnp.float32
BF16 = jnp.bfloat16


def kernel(
    n, n_tp, slots, tokens_ref, gain_ref, chosen_ref, weight_ref, gate_hbm, up_hbm, down_hbm, out_ref,
    gate_v, up_v, down_v, nbuf, xall, xs, sbuf, rbuf, hbuf, mix, obuf, pbuf, sumbuf, fbuf,
    w_sem, d_send, d_recv, c_send, c_recv, r_send, r_recv, g_send, g_recv, p_send, p_recv, f_send, f_recv,
):
    experts, depth, ff = gate_v.shape
    rows = tokens_ref.shape[0]
    subs, width = sbuf.shape[1], sbuf.shape[3]
    half = subs // 2
    group = n // experts
    ratio = n // n_tp
    me = lax.axis_index("ep")
    col = lax.axis_index("tp")

    odd = me % 2
    pos = (1 - odd) * (me // 2) + odd * (n - 1 - me // 2)

    def index_at(position):
        p = (position + 2 * n) % n
        late = p // (n // 2)
        return (1 - late) * 2 * p + late * (2 * (n - 1 - p) + 1)

    neighbour = (index_at(pos + 1), index_at(pos - 1))
    owner_col = me // ratio
    core = col % 2
    partner = col + 1 - 2 * core
    pairs = n_tp // 2
    own_slot = (me % ratio) * pairs + col // 2
    part_rows = rows // 2
    selfish = ((owner_col == col) & (me % 2 == core)).astype(jnp.int32)

    barrier = pltpu.get_barrier_semaphore()

    def greet(j, _):
        pl.semaphore_signal(barrier, inc=1, device_id=((me + j) % n, col), device_id_type=MESH)
        return 0

    lax.fori_loop(1, n, greet, 0)

    pl.semaphore_signal(barrier, inc=1, device_id=(me, partner), device_id_type=MESH)

    def owner_at(j):
        return ((me // 2 + n // 2 - 1 - j) % (n // 2)) * 2 + core

    def source_at(j):
        return col * ratio + j // pairs, (j % pairs) * 2 + me % 2

    def greet_out(j, _):
        target = owner_at(j)
        source_row, source_col = source_at(j)

        @pl.when((target != me) | (owner_col != col))
        def _():
            pl.semaphore_signal(barrier, inc=1, device_id=(target, owner_col), device_id_type=MESH)

        @pl.when((source_row != me) | (source_col != col))
        def _():
            pl.semaphore_signal(barrier, inc=1, device_id=(source_row, source_col), device_id_type=MESH)

        return 0

    lax.fori_loop(0, n // 2, greet_out, 0)

    loads = [
        pltpu.make_async_copy(gate_hbm, gate_v, w_sem.at[0]),
        pltpu.make_async_copy(up_hbm, up_v, w_sem.at[1]),
        pltpu.make_async_copy(down_hbm, down_v, w_sem.at[2]),
    ]
    for load in loads:
        load.start()

    my_rows = pl.ds(pl.multiple_of(core * part_rows, part_rows), part_rows)
    values = tokens_ref[my_rows, :].astype(F32)
    scale = lax.rsqrt(jnp.mean(values * values, axis=1, keepdims=True) + EPSILON)
    normed = (values * scale * gain_ref[...]).astype(BF16)
    for j in range(n):
        nbuf[j] = normed[:, j * depth : (j + 1) * depth]

    pl.semaphore_wait(barrier, n + 2 * (n // 2 - selfish))

    def dispatch(target, source):
        return pltpu.make_async_remote_copy(
            src_ref=nbuf.at[target], dst_ref=xall.at[source, core], send_sem=d_send.at[target],
            recv_sem=d_recv.at[source], device_id=(target, col), device_id_type=MESH,
        )

    def share(src, source, half_index):
        return pltpu.make_async_remote_copy(
            src_ref=src, dst_ref=xall.at[source, half_index], send_sem=c_send.at[source],
            recv_sem=c_recv.at[source], device_id=(me, partner), device_id_type=MESH,
        )

    def offset(j):
        late = j // (n // 2)
        return (1 - late) * (n // 2 + j) + late * (n - 1 - j)

    def send_tokens(j, _):
        dispatch((me + offset(j)) % n, me).start()
        return 0

    lax.fori_loop(0, n - 1, send_tokens, 0)
    share(nbuf.at[me], me, core).start()
    xall[me, core] = nbuf[me]
    mix[...] = jnp.zeros_like(mix)

    def pass_tokens(j, _):
        source = (me + n - offset(j)) % n
        dispatch(me, source).wait_recv()
        share(xall.at[source, core], source, core).start()
        return 0

    lax.fori_loop(0, n - 1, pass_tokens, 0)

    def wait_tokens(j, _):
        source = (me + n - j) % n
        share(xall.at[source, core], source, 1 - core).wait_recv()
        return 0

    lax.fori_loop(0, n, wait_tokens, 0)

    def piece_row(ref, q):
        start = pl.multiple_of((q % group) * slots, slots)
        return ref[pl.ds(q // group, 1), pl.ds(start, slots)]

    blocks = n * rows // 128
    step_blocks = min(blocks, 8)

    def gather(q):
        picked = jnp.transpose(jnp.broadcast_to(piece_row(chosen_ref, q), (128, slots)))
        lanes = lax.broadcasted_iota(jnp.int32, (slots, 128), 1)
        total = jnp.zeros((slots, depth), F32)
        per = step_blocks * 128 // rows
        for b in range(0, blocks, step_blocks):
            onehot = jnp.concatenate(
                [jnp.where(picked == lanes + (b + c) * 128, 1.0, 0.0).astype(BF16) for c in range(step_blocks)], axis=1
            )
            first = b * 128 // rows
            part = xall[first : first + per].reshape(step_blocks * 128, depth)
            total = total + jnp.dot(onehot, part, preferred_element_type=F32)
        xs[q] = total.astype(BF16)

    weights = (gate_v, up_v)

    def partial(direction, q, sub):
        w = weights[direction][q // group, :, sub * width : (sub + 1) * width]
        return jnp.dot(xs[q], w, preferred_element_type=F32)

    def reduce_copy(direction, src, step, sub):
        return pltpu.make_async_remote_copy(
            src_ref=src, dst_ref=rbuf.at[direction, step, sub], send_sem=r_send.at[direction, step, sub],
            recv_sem=r_recv.at[direction, step, sub], device_id=(neighbour[direction], col), device_id_type=MESH,
        )

    def chunk(direction, step):
        return index_at(pos - 1 - step) if direction == 0 else index_at(pos + 1 + step)

    loads[0].wait()
    loads[1].wait()
    for sub in range(subs):
        for direction in range(2):
            if sub == 0:
                gather(chunk(direction, 0))
            sbuf[direction, sub] = partial(direction, chunk(direction, 0), sub).astype(BF16)
            reduce_copy(direction, sbuf.at[direction, sub], 0, sub).start()

    def gather_rest(j, _):
        gather(index_at(pos - 1 - j))
        return 0

    lax.fori_loop(1, n - 2, gather_rest, 0)
    gather(me)

    def reduce_step(step, _):
        for sub in range(subs):
            for direction in range(2):
                mine = partial(direction, chunk(direction, step), sub)
                here = rbuf.at[direction, step - 1, sub]
                reduce_copy(direction, here, step - 1, sub).wait_recv()
                here[...] = (here[...].astype(F32) + mine).astype(BF16)
                reduce_copy(direction, here, step, sub).start()
        return 0

    lax.fori_loop(1, n - 1, reduce_step, 0)

    def spread_copy(direction, source, step, sub):
        block = hbuf.at[source, sub]
        return pltpu.make_async_remote_copy(
            src_ref=block, dst_ref=block, send_sem=g_send.at[step, sub], recv_sem=g_recv.at[step, sub],
            device_id=(neighbour[direction], col), device_id_type=MESH,
        )

    slot_scale = jnp.transpose(jnp.broadcast_to(piece_row(weight_ref, me), (128, slots)))
    slot_scale = jnp.concatenate([slot_scale] * (width // 128), axis=1)
    order = [s for pair in zip(range(half), range(half, subs)) for s in pair]
    for sub in order:
        parts = []
        for direction in range(2):
            mine = partial(direction, me, sub)
            here = rbuf.at[direction, n - 2, sub]
            reduce_copy(direction, here, n - 2, sub).wait_recv()
            parts.append(here[...].astype(F32) + mine)
        hbuf[me, sub] = (parts[0] / (1.0 + jnp.exp(-parts[0])) * parts[1] * slot_scale).astype(BF16)
        spread_copy(sub // half, me, 0, sub).start()
    loads[2].wait()

    def down(q, direction):
        total = jnp.zeros((slots, depth), F32)
        for sub in range(direction * half, (direction + 1) * half):
            w = down_v[q // group, :, sub * width : (sub + 1) * width]
            total = total + lax.dot_general(
                hbuf[q, sub], w, (((1,), (1,)), ((), ())), preferred_element_type=F32
            )
        return total.astype(BF16)

    def project(q, direction):
        picked = piece_row(chosen_ref, q)
        value = down(q, direction)
        size = step_blocks * 128
        for b in range(0, n * rows, size):
            numbers = lax.broadcasted_iota(jnp.int32, (size, slots), 0) + b
            onehot = jnp.where(numbers == picked, 1.0, 0.0).astype(BF16)
            mix[b : b + size] += jnp.dot(onehot, value, preferred_element_type=F32)

    def spread_step(step, _):
        for t in range(half):
            for direction in range(2):
                sub = direction * half + t
                source = chunk(direction, step - 1)
                spread_copy(direction, source, step - 1, sub).wait_recv()

                @pl.when(step < n - 1)
                def _():
                    spread_copy(direction, source, step, sub).start()

            for direction in range(2):
                if direction % half == t:
                    project(chunk(direction, step - 2), direction)
        return 0

    lax.fori_loop(1, n, spread_step, 0)

    last = (chunk(0, n - 2), chunk(1, n - 2))
    for direction in range(2):
        xs[direction] = down(last[direction], direction)

    def mix_rows(target):
        start = pl.multiple_of(target * rows, rows)
        numbers = lax.broadcasted_iota(jnp.int32, (rows, slots), 0) + start
        onehot = jnp.concatenate(
            [jnp.where(numbers == piece_row(chosen_ref, q), 1.0, 0.0).astype(BF16) for q in last], axis=1
        )
        late = jnp.dot(onehot, xs[0:2].reshape(2 * slots, depth), preferred_element_type=F32)
        return mix[pl.ds(start, rows), :] + late

    def pair_copy(j):
        return pltpu.make_async_remote_copy(
            src_ref=obuf.at[j], dst_ref=pbuf.at[j], send_sem=p_send.at[j],
            recv_sem=p_recv.at[j], device_id=(me, partner), device_id_type=MESH,
        )

    def final_copy(j, slot):
        return pltpu.make_async_remote_copy(
            src_ref=sumbuf.at[j], dst_ref=fbuf.at[slot], send_sem=f_send.at[j],
            recv_sem=f_recv.at[slot], device_id=(owner_at(j), owner_col), device_id_type=MESH,
        )

    def send_pair(j, _):
        obuf[j] = mix_rows(owner_at(j) + 1 - 2 * core).astype(BF16)
        pair_copy(j).start()
        return 0

    lax.fori_loop(0, n // 2, send_pair, 0)

    def send_out(j, _):
        target = owner_at(j)
        pair_copy(j).wait_recv()
        sumbuf[j] = (mix_rows(target) + pbuf[j].astype(F32)).astype(BF16)
        away = (target != me) | (owner_col != col)

        @pl.when(away)
        def _():
            final_copy(j, own_slot).start()

        @pl.when(jnp.logical_not(away))
        def _():
            fbuf[own_slot] = sumbuf[j]

        return 0

    lax.fori_loop(0, n // 2, send_out, 0)

    def sent_tokens(j, _):
        source = (me + j) % n
        share(xall.at[source, core], source, core).wait_send()

        @pl.when(j > 0)
        def _():
            dispatch(source, me).wait_send()

        return 0

    lax.fori_loop(0, n, sent_tokens, 0)

    def sent_ring(step, _):
        for sub in range(subs):
            for direction in range(2):
                reduce_copy(direction, sbuf.at[direction, sub], step, sub).wait_send()
            spread_copy(sub // half, me, step, sub).wait_send()
        return 0

    lax.fori_loop(0, n - 1, sent_ring, 0)

    def arrive(j, _):
        source_row, source_col = source_at(j)

        @pl.when((source_row != me) | (source_col != col))
        def _():
            final_copy(0, j).wait_recv()

        return 0

    lax.fori_loop(0, n // 2, arrive, 0)
    for b in range(ratio):
        total = fbuf[b * pairs].astype(F32)
        for k in range(1, pairs):
            total = total + fbuf[b * pairs + k].astype(F32)
        out_ref[:, b * depth : (b + 1) * depth] = total.astype(BF16)

    def sent_out(j, _):
        pair_copy(j).wait_send()

        @pl.when((owner_at(j) != me) | (owner_col != col))
        def _():
            final_copy(j, own_slot).wait_send()

        return 0

    lax.fori_loop(0, n // 2, sent_out, 0)


def body(tokens, norm_gain, chosen, slot_weight, gate_weight, up_weight, down_weight):
    n = lax.axis_size("ep")
    n_tp = lax.axis_size("tp")
    rows, model_width = tokens.shape
    experts, depth, ff = gate_weight.shape
    slots = chosen.shape[0] * chosen.shape[1] // n
    width = max(128, ff // 4)
    subs = ff // width
    vmem = pl.BlockSpec(memory_space=pltpu.VMEM)
    anywhere = pl.BlockSpec(memory_space=pl.ANY)
    dma = pltpu.SemaphoreType.DMA
    return pl.pallas_call(
        functools.partial(kernel, n, n_tp, slots),
        out_shape=jax.ShapeDtypeStruct((rows, model_width // n_tp), BF16),
        in_specs=[vmem] * 4 + [anywhere] * 3,
        out_specs=vmem,
        scratch_shapes=[
            pltpu.VMEM((experts, depth, ff), BF16),
            pltpu.VMEM((experts, depth, ff), BF16),
            pltpu.VMEM((experts, depth, ff), BF16),
            pltpu.VMEM((n, rows // 2, depth), BF16),
            pltpu.VMEM((n, 2, rows // 2, depth), BF16),
            pltpu.VMEM((n, slots, depth), BF16),
            pltpu.VMEM((2, subs, slots, width), BF16),
            pltpu.VMEM((2, n - 1, subs, slots, width), BF16),
            pltpu.VMEM((n, subs, slots, width), BF16),
            pltpu.VMEM((n * rows, depth), F32),
            pltpu.VMEM((n // 2, rows, depth), BF16),
            pltpu.VMEM((n // 2, rows, depth), BF16),
            pltpu.VMEM((n // 2, rows, depth), BF16),
            pltpu.VMEM((n // 2, rows, depth), BF16),
            dma((3,)),
            dma((n,)),
            dma((n,)),
            dma((n,)),
            dma((n,)),
            dma((2, n - 1, subs)),
            dma((2, n - 1, subs)),
            dma((n - 1, subs)),
            dma((n - 1, subs)),
            dma((n // 2,)),
            dma((n // 2,)),
            dma((n // 2,)),
            dma((n // 2,)),
        ],
        compiler_params=pltpu.CompilerParams(
            collective_id=0, has_side_effects=True, vmem_limit_bytes=64 * 1024 * 1024 - 96 * 1024
        ),
    )(tokens, norm_gain.reshape(1, model_width), chosen, slot_weight, gate_weight, up_weight, down_weight)


def solution(mesh):
    in_specs = (
        P("ep", None),
        P(),
        P(),
        P(),
        P(None, "ep", "tp"),
        P(None, "ep", "tp"),
        P(None, "ep", "tp"),
    )
    out_specs = P("ep", "tp")
    return jax.shard_map(body, mesh=mesh, in_specs=in_specs, out_specs=out_specs, check_vma=False)
```

```python
import functools

import jax
import jax.numpy as jnp
from jax import lax
from jax.experimental import pallas as pl
from jax.experimental.pallas import tpu as pltpu
from jax.sharding import PartitionSpec as P

EPSILON = 1e-06
MESH = pl.DeviceIdType.MESH
F32 = jnp.float32
BF16 = jnp.bfloat16


def kernel(
    n, n_tp, slots, tokens_ref, gain_ref, chosen_ref, weight_ref, gate_hbm, up_hbm, down_hbm, out_ref,
    gate_v, up_v, down_v, nbuf, xall, xs, sbuf, rbuf, hbuf, mix, obuf, pbuf, sumbuf, fbuf,
    w_sem, d_send, d_recv, c_send, c_recv, r_send, r_recv, g_send, g_recv, p_send, p_recv, f_send, f_recv,
):
    experts, depth, ff = gate_v.shape
    rows = tokens_ref.shape[0]
    subs, width = sbuf.shape[1], sbuf.shape[3]
    half = subs // 2
    group = n // experts
    ratio = n // n_tp
    me = lax.axis_index("ep")
    col = lax.axis_index("tp")

    odd = me % 2
    pos = (1 - odd) * (me // 2) + odd * (n - 1 - me // 2)

    def index_at(position):
        p = (position + 2 * n) % n
        late = p // (n // 2)
        return (1 - late) * 2 * p + late * (2 * (n - 1 - p) + 1)

    neighbour = (index_at(pos + 1), index_at(pos - 1))
    owner_col = me // ratio
    core = col % 2
    partner = col + 1 - 2 * core
    pairs = n_tp // 2
    own_slot = (me % ratio) * pairs + col // 2
    part_rows = rows // 2
    selfish = ((owner_col == col) & (me % 2 == core)).astype(jnp.int32)

    barrier = pltpu.get_barrier_semaphore()

    def greet(j, _):
        pl.semaphore_signal(barrier, inc=1, device_id=((me + j) % n, col), device_id_type=MESH)
        return 0

    lax.fori_loop(1, n, greet, 0)

    pl.semaphore_signal(barrier, inc=1, device_id=(me, partner), device_id_type=MESH)

    def owner_at(j):
        return ((me // 2 + n // 2 - 1 - j) % (n // 2)) * 2 + core

    def source_at(j):
        return col * ratio + j // pairs, (j % pairs) * 2 + me % 2

    def greet_out(j, _):
        target = owner_at(j)
        source_row, source_col = source_at(j)

        @pl.when((target != me) | (owner_col != col))
        def _():
            pl.semaphore_signal(barrier, inc=1, device_id=(target, owner_col), device_id_type=MESH)

        @pl.when((source_row != me) | (source_col != col))
        def _():
            pl.semaphore_signal(barrier, inc=1, device_id=(source_row, source_col), device_id_type=MESH)

        return 0

    lax.fori_loop(0, n // 2, greet_out, 0)

    loads = [
        pltpu.make_async_copy(gate_hbm, gate_v, w_sem.at[0]),
        pltpu.make_async_copy(up_hbm, up_v, w_sem.at[1]),
        pltpu.make_async_copy(down_hbm, down_v, w_sem.at[2]),
    ]
    for load in loads:
        load.start()

    my_rows = pl.ds(pl.multiple_of(core * part_rows, part_rows), part_rows)
    values = tokens_ref[my_rows, :].astype(F32)
    scale = lax.rsqrt(jnp.mean(values * values, axis=1, keepdims=True) + EPSILON)
    normed = (values * scale * gain_ref[...]).astype(BF16)
    for j in range(n):
        nbuf[j] = normed[:, j * depth : (j + 1) * depth]

    pl.semaphore_wait(barrier, n + 2 * (n // 2 - selfish))

    def dispatch(target, source):
        return pltpu.make_async_remote_copy(
            src_ref=nbuf.at[target], dst_ref=xall.at[source, core], send_sem=d_send.at[target],
            recv_sem=d_recv.at[source], device_id=(target, col), device_id_type=MESH,
        )

    def share(src, source, half_index):
        return pltpu.make_async_remote_copy(
            src_ref=src, dst_ref=xall.at[source, half_index], send_sem=c_send.at[source],
            recv_sem=c_recv.at[source], device_id=(me, partner), device_id_type=MESH,
        )

    def offset(j):
        late = j // (n // 2)
        return (1 - late) * (n // 2 + j) + late * (n - 1 - j)

    def send_tokens(j, _):
        dispatch((me + offset(j)) % n, me).start()
        return 0

    lax.fori_loop(0, n - 1, send_tokens, 0)
    share(nbuf.at[me], me, core).start()
    xall[me, core] = nbuf[me]
    mix[...] = jnp.zeros_like(mix)

    def pass_tokens(j, _):
        source = (me + n - offset(j)) % n
        dispatch(me, source).wait_recv()
        share(xall.at[source, core], source, core).start()
        return 0

    lax.fori_loop(0, n - 1, pass_tokens, 0)

    def wait_tokens(j, _):
        source = (me + n - j) % n
        share(xall.at[source, core], source, 1 - core).wait_recv()
        return 0

    lax.fori_loop(0, n, wait_tokens, 0)

    def piece_row(ref, q):
        start = pl.multiple_of((q % group) * slots, slots)
        return ref[pl.ds(q // group, 1), pl.ds(start, slots)]

    blocks = n * rows // 128
    step_blocks = min(blocks, 8)

    def gather(q):
        picked = jnp.transpose(jnp.broadcast_to(piece_row(chosen_ref, q), (128, slots)))
        lanes = lax.broadcasted_iota(jnp.int32, (slots, 128), 1)
        total = jnp.zeros((slots, depth), F32)
        per = step_blocks * 128 // rows
        for b in range(0, blocks, step_blocks):
            onehot = jnp.concatenate(
                [jnp.where(picked == lanes + (b + c) * 128, 1.0, 0.0).astype(BF16) for c in range(step_blocks)], axis=1
            )
            first = b * 128 // rows
            part = xall[first : first + per].reshape(step_blocks * 128, depth)
            total = total + jnp.dot(onehot, part, preferred_element_type=F32)
        xs[q] = total.astype(BF16)

    weights = (gate_v, up_v)

    def partial(direction, q, sub):
        w = weights[direction][q // group, :, sub * width : (sub + 1) * width]
        return jnp.dot(xs[q], w, preferred_element_type=F32)

    def reduce_copy(direction, src, step, sub):
        return pltpu.make_async_remote_copy(
            src_ref=src, dst_ref=rbuf.at[direction, step, sub], send_sem=r_send.at[direction, step, sub],
            recv_sem=r_recv.at[direction, step, sub], device_id=(neighbour[direction], col), device_id_type=MESH,
        )

    def chunk(direction, step):
        return index_at(pos - 1 - step) if direction == 0 else index_at(pos + 1 + step)

    loads[0].wait()
    loads[1].wait()
    for sub in range(subs):
        for direction in range(2):
            if sub == 0:
                gather(chunk(direction, 0))
            sbuf[direction, sub] = partial(direction, chunk(direction, 0), sub).astype(BF16)
            reduce_copy(direction, sbuf.at[direction, sub], 0, sub).start()

    def gather_rest(j, _):
        gather(index_at(pos - 1 - j))
        return 0

    lax.fori_loop(1, n - 2, gather_rest, 0)
    gather(me)

    def reduce_step(step, _):
        for sub in range(subs):
            for direction in range(2):
                mine = partial(direction, chunk(direction, step), sub)
                here = rbuf.at[direction, step - 1, sub]
                reduce_copy(direction, here, step - 1, sub).wait_recv()
                here[...] = (here[...].astype(F32) + mine).astype(BF16)
                reduce_copy(direction, here, step, sub).start()
        return 0

    lax.fori_loop(1, n - 1, reduce_step, 0)

    bands = 2
    band_rows = slots // bands

    def spread_copy(direction, source, step, sub, band):
        block = hbuf.at[source, sub, pl.ds(band * band_rows, band_rows)]
        return pltpu.make_async_remote_copy(
            src_ref=block, dst_ref=block, send_sem=g_send.at[step, sub, band], recv_sem=g_recv.at[step, sub, band],
            device_id=(neighbour[direction], col), device_id_type=MESH,
        )

    slot_scale = jnp.transpose(jnp.broadcast_to(piece_row(weight_ref, me), (128, slots)))
    slot_scale = jnp.concatenate([slot_scale] * (width // 128), axis=1)
    order = [s for pair in zip(range(half), range(half, subs)) for s in pair]
    for sub in order:
        parts = []
        for direction in range(2):
            mine = partial(direction, me, sub)
            here = rbuf.at[direction, n - 2, sub]
            reduce_copy(direction, here, n - 2, sub).wait_recv()
            parts.append(here[...].astype(F32) + mine)
        hbuf[me, sub] = (parts[0] / (1.0 + jnp.exp(-parts[0])) * parts[1] * slot_scale).astype(BF16)
        for band in range(bands):
            spread_copy(sub // half, me, 0, sub, band).start()
    loads[2].wait()

    def down(q, direction):
        total = jnp.zeros((slots, depth), F32)
        for sub in range(direction * half, (direction + 1) * half):
            w = down_v[q // group, :, sub * width : (sub + 1) * width]
            total = total + lax.dot_general(
                hbuf[q, sub], w, (((1,), (1,)), ((), ())), preferred_element_type=F32
            )
        return total.astype(BF16)

    def project(q, direction):
        picked = piece_row(chosen_ref, q)
        value = down(q, direction)
        size = step_blocks * 128
        for b in range(0, n * rows, size):
            numbers = lax.broadcasted_iota(jnp.int32, (size, slots), 0) + b
            onehot = jnp.where(numbers == picked, 1.0, 0.0).astype(BF16)
            mix[b : b + size] += jnp.dot(onehot, value, preferred_element_type=F32)

    def spread_step(step, _):
        for t in range(half):
            for band, direction in ((0, 0), (0, 1), (1, 0), (1, 1)):
                sub = direction * half + t
                source = chunk(direction, step - 1)
                spread_copy(direction, source, step - 1, sub, band).wait_recv()

                @pl.when(step < n - 1)
                def _():
                    spread_copy(direction, source, step, sub, band).start()

            for direction in range(2):
                if direction % half == t:
                    project(chunk(direction, step - 2), direction)
        return 0

    lax.fori_loop(1, n, spread_step, 0)

    last = (chunk(0, n - 2), chunk(1, n - 2))
    for direction in range(2):
        xs[direction] = down(last[direction], direction)

    def mix_rows(target):
        start = pl.multiple_of(target * rows, rows)
        numbers = lax.broadcasted_iota(jnp.int32, (rows, slots), 0) + start
        onehot = jnp.concatenate(
            [jnp.where(numbers == piece_row(chosen_ref, q), 1.0, 0.0).astype(BF16) for q in last], axis=1
        )
        late = jnp.dot(onehot, xs[0:2].reshape(2 * slots, depth), preferred_element_type=F32)
        return mix[pl.ds(start, rows), :] + late

    def pair_copy(j):
        return pltpu.make_async_remote_copy(
            src_ref=obuf.at[j], dst_ref=pbuf.at[j], send_sem=p_send.at[j],
            recv_sem=p_recv.at[j], device_id=(me, partner), device_id_type=MESH,
        )

    def final_copy(j, slot):
        return pltpu.make_async_remote_copy(
            src_ref=sumbuf.at[j], dst_ref=fbuf.at[slot], send_sem=f_send.at[j],
            recv_sem=f_recv.at[slot], device_id=(owner_at(j), owner_col), device_id_type=MESH,
        )

    def send_pair(j, _):
        obuf[j] = mix_rows(owner_at(j) + 1 - 2 * core).astype(BF16)
        pair_copy(j).start()
        return 0

    lax.fori_loop(0, n // 2, send_pair, 0)

    def send_out(j, _):
        target = owner_at(j)
        pair_copy(j).wait_recv()
        sumbuf[j] = (mix_rows(target) + pbuf[j].astype(F32)).astype(BF16)
        away = (target != me) | (owner_col != col)

        @pl.when(away)
        def _():
            final_copy(j, own_slot).start()

        @pl.when(jnp.logical_not(away))
        def _():
            fbuf[own_slot] = sumbuf[j]

        return 0

    lax.fori_loop(0, n // 2, send_out, 0)

    def sent_tokens(j, _):
        source = (me + j) % n
        share(xall.at[source, core], source, core).wait_send()

        @pl.when(j > 0)
        def _():
            dispatch(source, me).wait_send()

        return 0

    lax.fori_loop(0, n, sent_tokens, 0)

    def sent_ring(step, _):
        for sub in range(subs):
            for direction in range(2):
                reduce_copy(direction, sbuf.at[direction, sub], step, sub).wait_send()
            for band in range(bands):
                spread_copy(sub // half, me, step, sub, band).wait_send()
        return 0

    lax.fori_loop(0, n - 1, sent_ring, 0)

    def arrive(j, _):
        source_row, source_col = source_at(j)

        @pl.when((source_row != me) | (source_col != col))
        def _():
            final_copy(0, j).wait_recv()

        return 0

    lax.fori_loop(0, n // 2, arrive, 0)
    for b in range(ratio):
        total = fbuf[b * pairs].astype(F32)
        for k in range(1, pairs):
            total = total + fbuf[b * pairs + k].astype(F32)
        out_ref[:, b * depth : (b + 1) * depth] = total.astype(BF16)

    def sent_out(j, _):
        pair_copy(j).wait_send()

        @pl.when((owner_at(j) != me) | (owner_col != col))
        def _():
            final_copy(j, own_slot).wait_send()

        return 0

    lax.fori_loop(0, n // 2, sent_out, 0)


def body(tokens, norm_gain, chosen, slot_weight, gate_weight, up_weight, down_weight):
    n = lax.axis_size("ep")
    n_tp = lax.axis_size("tp")
    rows, model_width = tokens.shape
    experts, depth, ff = gate_weight.shape
    slots = chosen.shape[0] * chosen.shape[1] // n
    width = max(128, ff // 4)
    subs = ff // width
    vmem = pl.BlockSpec(memory_space=pltpu.VMEM)
    anywhere = pl.BlockSpec(memory_space=pl.ANY)
    dma = pltpu.SemaphoreType.DMA
    return pl.pallas_call(
        functools.partial(kernel, n, n_tp, slots),
        out_shape=jax.ShapeDtypeStruct((rows, model_width // n_tp), BF16),
        in_specs=[vmem] * 4 + [anywhere] * 3,
        out_specs=vmem,
        scratch_shapes=[
            pltpu.VMEM((experts, depth, ff), BF16),
            pltpu.VMEM((experts, depth, ff), BF16),
            pltpu.VMEM((experts, depth, ff), BF16),
            pltpu.VMEM((n, rows // 2, depth), BF16),
            pltpu.VMEM((n, 2, rows // 2, depth), BF16),
            pltpu.VMEM((n, slots, depth), BF16),
            pltpu.VMEM((2, subs, slots, width), BF16),
            pltpu.VMEM((2, n - 1, subs, slots, width), BF16),
            pltpu.VMEM((n, subs, slots, width), BF16),
            pltpu.VMEM((n * rows, depth), F32),
            pltpu.VMEM((n // 2, rows, depth), BF16),
            pltpu.VMEM((n // 2, rows, depth), BF16),
            pltpu.VMEM((n // 2, rows, depth), BF16),
            pltpu.VMEM((n // 2, rows, depth), BF16),
            dma((3,)),
            dma((n,)),
            dma((n,)),
            dma((n,)),
            dma((n,)),
            dma((2, n - 1, subs)),
            dma((2, n - 1, subs)),
            dma((n - 1, subs, 2)),
            dma((n - 1, subs, 2)),
            dma((n // 2,)),
            dma((n // 2,)),
            dma((n // 2,)),
            dma((n // 2,)),
        ],
        compiler_params=pltpu.CompilerParams(
            collective_id=0, has_side_effects=True, vmem_limit_bytes=64 * 1024 * 1024 - 96 * 1024
        ),
    )(tokens, norm_gain.reshape(1, model_width), chosen, slot_weight, gate_weight, up_weight, down_weight)


def solution(mesh):
    in_specs = (
        P("ep", None),
        P(),
        P(),
        P(),
        P(None, "ep", "tp"),
        P(None, "ep", "tp"),
        P(None, "ep", "tp"),
    )
    out_specs = P("ep", "tp")
    return jax.shard_map(body, mesh=mesh, in_specs=in_specs, out_specs=out_specs, check_vma=False)
```
